32 devices in a mesh: sp: 8 (over z, x), dp: 4 (over y, core).
Axes of the slice: x: 2, y: 2, z: 4, core: 2. Of those that a mesh axis runs over, the one named last changes fastest.
Arguments:
- tokens: bfloat16 [4, 3072, 2048], P('dp', 'sp'), may hold values from -6 to 6
- q_weight: bfloat16 [2048, 1024], P(('sp', 'dp')), may hold values from -0.13258252 to 0.13258252
- k_weight: bfloat16 [2048, 256], P(('sp', 'dp')), may hold values from -0.13258252 to 0.13258252
- v_weight: bfloat16 [2048, 256], P(('sp', 'dp')), may hold values from -0.125 to 0.125
- out_weight: bfloat16 [1024, 2048], P(None, ('sp', 'dp')), may hold values from -6 to 6
- q_gain: float32 [64], replicated, may hold values from 0.5 to 8
- k_gain: float32 [64], replicated, may hold values from 0.5 to 8
Outputs:
- mixed: bfloat16 [4, 3072, 2048], P('dp', 'sp')
The draws below stay inside these ranges and needn't reach their ends.
All inputs are finite; a program needn't handle non-finite values.
Results may differ from the reference program's by a relative error of at most 0.0055.
The reference program's roundings to bfloat16 on the way (of `values`, `shares` and `attended`) count: a program that leaves them out, or rounds other values in their place, can miss the bound.
Values may be sent and summed in bfloat16 or wider, within the bound.
A program may use at most 128 MiB of HBM per device.

```python
import math
import jax
import jax.numpy as jnp
from jax import lax

D = 2048
Q_HEADS = 16
KV_HEADS = 4
HEAD_DIM = 64
GRID_W = 64
GROUP = 4
SEQ = 3072
BATCH = 4


def draw_pair(key):
    query_draw = jnp.clip(jax.random.normal(jax.random.fold_in(key, 11), (D, Q_HEADS * HEAD_DIM), jnp.float32), -6.0, 6.0) / math.sqrt(D)
    key_draw = jnp.clip(jax.random.normal(jax.random.fold_in(key, 12), (D, KV_HEADS * HEAD_DIM), jnp.float32), -6.0, 6.0) / math.sqrt(D)
    return (query_draw, key_draw)


def draw_q_weight(key, part):
    return draw_pair(key)[0].astype(jnp.bfloat16)


def draw_k_weight(key, part):
    return draw_pair(key)[1].astype(jnp.bfloat16)


def draw_gain(key):
    return 1.0 + 0.18 * jnp.clip(jax.random.normal(key, (HEAD_DIM,), jnp.float32), -2.5, 2.5)


def draw_q_gain(key, part):
    return draw_gain(jax.random.fold_in(key, 21))


def draw_k_gain(key, part):
    return draw_gain(jax.random.fold_in(key, 22))


def steps_of(rng, dims, shards, smallest, largest):
    def one(axis_at, parts):
        steps = jax.random.uniform(jax.random.fold_in(jax.random.fold_in(rng, 6), axis_at), (parts,), jnp.float32, smallest / len(shards), largest / len(shards))
        return jnp.repeat(jnp.exp(steps), dims[axis_at] // parts).reshape((-1,) + (1,) * (len(dims) - axis_at - 1))

    gain = one(*shards[0])
    for cut in shards[1:]:
        gain = gain * one(*cut)
    return gain


def noise(rng, shape, scale, limit, pieces=(), kind=jnp.bfloat16):
    array = jax.random.normal(rng, shape, jnp.float32) * scale
    if len(pieces) > 0:
        array = steps_of(rng, shape, pieces, -0.22, 0.18) * array
    return jnp.clip(array, min=-limit, max=limit).astype(kind)


def setup_inputs(seed: int = 0) -> dict:
    key_list = jax.random.split(jax.random.key(seed), 8)
    return {
        "tokens": noise(key_list[0], (BATCH, SEQ, D), 1.0, 6.0, ((0, 4), (1, 8))),
        "q_weight": draw_q_weight(jax.random.fold_in(key_list[7], 71), 0),
        "k_weight": draw_k_weight(jax.random.fold_in(key_list[7], 71), 0),
        "v_weight": noise(key_list[3], (D, KV_HEADS * HEAD_DIM), D ** -0.5, 0.125, ((0, 32),)),
        "out_weight": noise(key_list[4], (Q_HEADS * HEAD_DIM, D), (32.0 / (Q_HEADS * HEAD_DIM) ** 0.5), 6.0, ((1, 32),)),
        "q_gain": draw_q_gain(jax.random.fold_in(key_list[7], 71), 0),
        "k_gain": draw_k_gain(jax.random.fold_in(key_list[7], 71), 0),
    }


epsilon = 1e-06
rope_base = 10000.0

def normalize(tensor, gain_vec):
    mean_sq = lax.optimization_barrier(jnp.mean(tensor * tensor, axis=-1, keepdims=True))
    return tensor * lax.rsqrt(mean_sq + epsilon) * gain_vec.astype(jnp.float32)

def rotate(tensor, offset):
    row_count = tensor.shape[0]
    head_width = tensor.shape[2]
    quarter = head_width // 4
    half_width = head_width // 2
    positions = jnp.arange(row_count, dtype=jnp.int32) + offset
    frequency = rope_base ** (-jnp.arange(quarter, dtype=jnp.float32) / quarter)

    def rotate_pair(segment, coords):
        angles = coords.astype(jnp.float32)[:, None] * frequency[None, :]
        cosine = jnp.cos(angles)[:, None, :]
        sine_val = jnp.sin(angles)[:, None, :]
        low_half = segment[..., :quarter]
        high_half = segment[..., quarter:]
        return jnp.concatenate([low_half * cosine - high_half * sine_val, high_half * cosine + low_half * sine_val], axis=-1)
    return jnp.concatenate([rotate_pair(tensor[..., :half_width], positions // GRID_W), rotate_pair(tensor[..., half_width:], positions % GRID_W)], axis=-1)

def attend(query_rows, key_rows, value_rows):
    row_count, head_width = query_rows.shape
    block_rows = math.gcd(row_count, 512)
    score_scale = head_width ** (-0.5)

    def attend_block(segment):
        scores = lax.dot_general(segment, key_rows, (((1,), (1,)), ((), ())), preferred_element_type=jnp.float32) * score_scale
        row_max = lax.optimization_barrier(jnp.max(scores, axis=-1, keepdims=True))
        weights = jnp.exp(scores - row_max)
        shares = (weights / lax.optimization_barrier(jnp.sum(weights, axis=-1, keepdims=True))).astype(jnp.bfloat16)
        return jnp.dot(shares, value_rows, preferred_element_type=jnp.float32).astype(jnp.bfloat16)
    blocks = query_rows.reshape(row_count // block_rows, block_rows, head_width)
    return lax.map(attend_block, blocks).reshape(row_count, head_width)

def reference(tokens, q_weight, k_weight, v_weight, out_weight, q_gain, k_gain):

    def sequence_out(rows_in):
        seq_len = rows_in.shape[0]
        query_raw = jnp.dot(rows_in, q_weight, preferred_element_type=jnp.float32).reshape(seq_len, Q_HEADS, HEAD_DIM)
        key_raw = jnp.dot(rows_in, k_weight, preferred_element_type=jnp.float32).reshape(seq_len, KV_HEADS, HEAD_DIM)
        value_raw = jnp.dot(rows_in, v_weight, preferred_element_type=jnp.float32).reshape(seq_len, KV_HEADS, HEAD_DIM)
        queries = rotate(normalize(query_raw, q_gain), 0).astype(jnp.bfloat16)
        keys = rotate(normalize(key_raw, k_gain), 0).astype(jnp.bfloat16)
        values = value_raw.astype(jnp.bfloat16)
        q_major = jnp.transpose(queries, (1, 0, 2))
        k_major = jnp.transpose(keys, (1, 0, 2))
        v_major = jnp.transpose(values, (1, 0, 2))

        def head_out(head_index):
            kv_index = head_index // GROUP
            q_rows = lax.dynamic_index_in_dim(q_major, head_index, 0, keepdims=False)
            k_rows = lax.dynamic_index_in_dim(k_major, kv_index, 0, keepdims=False)
            v_rows = lax.dynamic_index_in_dim(v_major, kv_index, 0, keepdims=False)
            return attend(q_rows, k_rows, v_rows)
        heads_done = lax.map(head_out, jnp.arange(Q_HEADS, dtype=jnp.int32))
        attended = jnp.transpose(heads_done, (1, 0, 2)).reshape(seq_len, Q_HEADS * HEAD_DIM)
        return jnp.dot(attended, out_weight, preferred_element_type=jnp.float32).astype(jnp.bfloat16)
    return lax.map(sequence_out, tokens)
```

```python
import functools
import math

import jax
import jax.numpy as jnp
from jax import lax
from jax.experimental import pallas as pl
from jax.experimental.pallas import tpu as pltpu
from jax.sharding import PartitionSpec as P

GRID_W = 64
CORES = 2
epsilon = 1e-06
rope_base = 10000.0
VMEM_BYTES = 60 * 1024 * 1024


def tables(tok_count, head_width, offset, width):
    quarter = head_width // 4
    positions = jnp.arange(tok_count, dtype=jnp.int32) + offset
    frequency = rope_base ** (-jnp.arange(quarter, dtype=jnp.float32) / quarter)
    row_angle = (positions // GRID_W).astype(jnp.float32)[:, None] * frequency[None, :]
    col_angle = (positions % GRID_W).astype(jnp.float32)[:, None] * frequency[None, :]
    cos = jnp.concatenate([jnp.cos(row_angle)] * 2 + [jnp.cos(col_angle)] * 2, axis=1)
    sin_r, sin_c = jnp.sin(row_angle), jnp.sin(col_angle)
    sin = jnp.concatenate([-sin_r, sin_r, -sin_c, sin_c], axis=1)
    return jnp.tile(cos, (1, width // head_width)), jnp.tile(sin, (1, width // head_width))


class Net:
    def __init__(self, dims):
        self.zs, self.xs, self.ys = dims
        sp, dp = lax.axis_index("sp"), lax.axis_index("dp")
        self.z, self.x = sp // self.xs, sp % self.xs
        self.y, self.c = dp // CORES, dp % CORES
        self.ox, self.oy, self.oc = 1 - self.x, 1 - self.y, 1 - self.c

    def at(self, z=None, x=None, y=None, c=None):
        z = self.z if z is None else z
        x = self.x if x is None else x
        y = self.y if y is None else y
        c = self.c if c is None else c
        return {"sp": z * self.xs + x, "dp": y * CORES + c}

    def sides(self):
        return ((-1, 1), (1, -1))

    def inside(self, z):
        return jnp.logical_and(z >= 0, z < self.zs)


def greet(net, fixed):
    barrier = pltpu.get_barrier_semaphore()
    for where in fixed:
        pl.semaphore_signal(barrier, inc=1, device_id=where, device_id_type=pl.DeviceIdType.MESH)
    for step in (-1, 1):

        @pl.when(net.inside(net.z + step))
        def _():
            pl.semaphore_signal(
                barrier,
                inc=1,
                device_id=net.at(z=net.z + step),
                device_id_type=pl.DeviceIdType.MESH,
            )

    along = jnp.minimum(net.z, 1) + jnp.minimum(net.zs - 1 - net.z, 1)
    pl.semaphore_wait(barrier, len(fixed) + along)


def remote(src, dst, send, recv, where):
    return pltpu.make_async_remote_copy(
        src_ref=src,
        dst_ref=dst,
        send_sem=send,
        recv_sem=recv,
        device_id=where,
        device_id_type=pl.DeviceIdType.MESH,
    )


def gather_weights(net, w_own, wbuf, own_sem, zs_sem, zr_sem, xs, xr, ys, yr, ds, dr, cs, cr):
    half = wbuf.shape[-1] // 2
    halves = (pl.ds(0, half), pl.ds(half, half))

    def block(z, x, y, c):
        return wbuf.at[z, x, y, c]

    def part(z, x, y, c, h):
        return wbuf.at[z, x, y, c, :, halves[h]]

    def to_x(k, z, src=None):
        dst = block(z, net.x, net.y, net.c)
        return remote(dst if src is None else src, dst, xs.at[k], xr.at[k], net.at(x=net.ox))

    def from_x(k, z):
        b = block(z, net.ox, net.y, net.c)
        return remote(b, b, xs.at[k], xr.at[k], net.at(x=net.ox))

    def to_y(k, z, src=None):
        dst = block(z, net.x, net.y, net.c)
        return remote(dst if src is None else src, dst, ys.at[k], yr.at[k], net.at(y=net.oy))

    def from_y(k, z):
        b = block(z, net.x, net.oy, net.c)
        return remote(b, b, ys.at[k], yr.at[k], net.at(y=net.oy))

    def diag_to(k, z, h):
        if h == 0:
            b = part(z, net.ox, net.y, net.c, 0)
            return remote(b, b, ds.at[0, k], dr.at[0, k], net.at(y=net.oy))
        b = part(z, net.x, net.oy, net.c, 1)
        return remote(b, b, ds.at[1, k], dr.at[1, k], net.at(x=net.ox))

    def diag_from(k, z, h):
        b = part(z, net.ox, net.oy, net.c, h)
        where = net.at(y=net.oy) if h == 0 else net.at(x=net.ox)
        return remote(b, b, ds.at[h, k], dr.at[h, k], where)

    def core(kind, k, z, c, src=None):
        x = net.ox if kind in (1, 3, 4) else net.x
        y = net.oy if kind in (2, 3, 4) else net.y
        b = part(z, x, y, c, kind - 3) if kind >= 3 else block(z, x, y, c)
        return remote(
            b if src is None else src, b, cs.at[kind, k], cr.at[kind, k], net.at(c=net.oc)
        )

    def to_z(k, z, step, src=None):
        dst = block(z, net.x, net.y, net.c)
        return remote(
            dst if src is None else src, dst, zs_sem.at[k], zr_sem.at[k], net.at(z=net.z + step)
        )

    def slots():
        for step in range(net.zs - 1):
            for side in range(2):
                sign = -1 if side == 0 else 1
                yield step, side, 1 + 2 * step + side, net.z + sign * (step + 1), -sign

    def spread(k, z, src=None):
        to_x(k, z, src).start()
        to_y(k, z, src).start()
        core(0, k, z, net.c, src).start()

    def second(k, z):
        from_x(k, z).wait_recv()
        diag_to(k, z, 0).start()
        core(1, k, z, net.c).start()
        from_y(k, z).wait_recv()
        diag_to(k, z, 1).start()
        core(2, k, z, net.c).start()

    def third(k, z):
        diag_from(k, z, 0).wait_recv()
        core(3, k, z, net.c).start()
        diag_from(k, z, 1).wait_recv()
        core(4, k, z, net.c).start()

    mine = pltpu.make_async_copy(w_own, block(net.z, net.x, net.y, net.c), own_sem)
    mine.start()
    for side, step in ((0, 1), (1, -1)):

        @pl.when(net.inside(net.z + step))
        def _():
            to_z(1 + side, net.z, step, w_own).start()

    spread(0, net.z, w_own)
    stages = [[(0, net.z)]]
    for s in range(net.zs - 1):
        here = []
        for step, side, k, z, onward in slots():
            if step != s:
                continue

            @pl.when(net.inside(z))
            def _():
                to_z(k, z, 0).wait_recv()
                if s < net.zs - 2:

                    @pl.when(net.inside(net.z + onward))
                    def _():
                        to_z(k + 2, z, onward).start()

                spread(k, z)

            here.append((k, z))
        for k, z in stages[-1]:

            @pl.when(net.inside(z))
            def _():
                second(k, z)

        if len(stages) > 1:
            for k, z in stages[-2]:

                @pl.when(net.inside(z))
                def _():
                    third(k, z)

        stages.append(here)
    for k, z in stages[-1]:

        @pl.when(net.inside(z))
        def _():
            second(k, z)

    for stage in stages[-2:]:
        for k, z in stage:

            @pl.when(net.inside(z))
            def _():
                third(k, z)

    for stage in stages:
        for k, z in stage:

            @pl.when(net.inside(z))
            def _():
                for kind in range(5):
                    core(kind, k, z, net.oc).wait_recv()

    def drain():
        mine.wait()
        for side, step in ((0, 1), (1, -1)):

            @pl.when(net.inside(net.z + step))
            def _():
                to_z(1 + side, net.z, step, w_own).wait_send()

        for step, side, k, z, onward in slots():
            if step < net.zs - 2:

                @pl.when(jnp.logical_and(net.inside(z), net.inside(net.z + onward)))
                def _():
                    to_z(k + 2, z, onward).wait_send()

        for stage in stages:
            for k, z in stage:

                @pl.when(net.inside(z))
                def _():
                    to_x(k, z).wait_send()
                    to_y(k, z).wait_send()
                    diag_to(k, z, 0).wait_send()
                    diag_to(k, z, 1).wait_send()
                    for kind in range(5):
                        core(kind, k, z, net.c).wait_send()

    drain()


def project_kernel(
    dims, scale, head_width, tok_ref, w_own, cos_ref, sin_ref, qg_ref, kg_ref, q_ref, kv_ref,
    wbuf, *sems
):
    net = Net(dims)
    greet(net, (net.at(x=net.ox), net.at(y=net.oy), net.at(c=net.oc)))
    gather_weights(net, w_own, wbuf, *sems)
    rows, width = cos_ref.shape
    depth = tok_ref.shape[1]
    kv_width = kv_ref.shape[1] // 2
    pair = 2 * head_width
    r = lax.broadcasted_iota(jnp.int32, (width, width), 0) // head_width
    c = lax.broadcasted_iota(jnp.int32, (width, width), 1) // head_width
    averager = jnp.where(r == c, 1.0 / head_width, 0.0).astype(jnp.float32)
    lane = lax.broadcasted_iota(jnp.int32, (rows, width), 1)
    first = lane % (head_width // 2) < head_width // 4
    low = lax.broadcasted_iota(jnp.int32, (rows, pair), 1) < head_width

    def product(at):
        w = wbuf[:, :, :, :, :, at : at + width].reshape(depth, width)
        return jnp.dot(tok_ref[...], w, preferred_element_type=jnp.float32)

    def turned(t, gain):
        mean_sq = jnp.dot(
            t * t, averager, precision=lax.Precision.HIGHEST, preferred_element_type=jnp.float32
        )
        t = t * lax.rsqrt(mean_sq + epsilon) * gain
        quarter = head_width // 4
        other = jnp.where(first, pltpu.roll(t, width - quarter, 1), pltpu.roll(t, quarter, 1))
        return t * cos_ref[...] + other * sin_ref[...]

    per = width // head_width
    for j in range(kv_width // width):
        k = turned(product(j * width), kg_ref[...])
        v = product(kv_width + j * width)
        for i in range(0, per, 2):
            kp = k[:, i * head_width : i * head_width + pair]
            vp = v[:, i * head_width : i * head_width + pair]
            at = (j * per + i) * pair
            kv_ref[:, at : at + pair] = jnp.where(low, kp, pltpu.roll(vp, head_width, 1)).astype(
                kv_ref.dtype
            )
            kv_ref[:, at + pair : at + 2 * pair] = jnp.where(
                low, pltpu.roll(kp, head_width, 1), vp
            ).astype(kv_ref.dtype)
    for j in range(q_ref.shape[0] // per):
        q = turned(product(2 * kv_width + j * width), qg_ref[...])
        q = q.astype(q_ref.dtype).astype(jnp.float32) * scale
        for i in range(0, per, 2):
            qp = q[:, i * head_width : i * head_width + pair]
            q_ref[j * per + i] = jnp.where(low, qp, 0.0).astype(q_ref.dtype)
            q_ref[j * per + i + 1] = jnp.where(low, pltpu.roll(qp, head_width, 1), 0.0).astype(
                q_ref.dtype
            )


def gather_kv(net, own, buf, own_sem, zs_sem, zr_sem, xs, xr):
    def block(z, x):
        return buf.at[z, x]

    def to_z(k, z, step, src=None):
        dst = block(z, net.x)
        return remote(
            dst if src is None else src, dst, zs_sem.at[k], zr_sem.at[k], net.at(z=net.z + step)
        )

    def to_x(k, z, src=None):
        dst = block(z, net.x)
        return remote(dst if src is None else src, dst, xs.at[k], xr.at[k], net.at(x=net.ox))

    def from_x(k, z):
        b = block(z, net.ox)
        return remote(b, b, xs.at[k], xr.at[k], net.at(x=net.ox))

    mine = pltpu.make_async_copy(own, block(net.z, net.x), own_sem)
    mine.start()
    to_x(0, net.z, own).start()
    for side, step in ((0, 1), (1, -1)):

        @pl.when(net.inside(net.z + step))
        def _():
            to_z(1 + side, net.z, step, own).start()

    slots = [
        (s, 1 + 2 * s + side, net.z + sign * (s + 1), -sign)
        for s in range(net.zs - 1)
        for side, sign in ((0, -1), (1, 1))
    ]
    for s, k, z, onward in slots:

        @pl.when(net.inside(z))
        def _():
            to_z(k, z, 0).wait_recv()
            if s < net.zs - 2:

                @pl.when(net.inside(net.z + onward))
                def _():
                    to_z(k + 2, z, onward).start()

            to_x(k, z).start()

    from_x(0, net.z).wait_recv()
    to_x(0, net.z, own).wait_send()
    mine.wait()
    for side, step in ((0, 1), (1, -1)):

        @pl.when(net.inside(net.z + step))
        def _():
            to_z(1 + side, net.z, step, own).wait_send()

    for s, k, z, onward in slots:

        @pl.when(net.inside(z))
        def _():
            from_x(k, z).wait_recv()
            to_x(k, z).wait_send()
            if s < net.zs - 2:

                @pl.when(net.inside(net.z + onward))
                def _():
                    to_z(k + 2, z, onward).wait_send()


def softmax_rows(q, keys, split):
    s = lax.dot_general(q, keys, (((1,), (1,)), ((), ())), preferred_element_type=jnp.float32)
    p = jnp.exp(s - jnp.max(s, axis=-1, keepdims=True))
    total = jnp.sum(p, axis=-1, keepdims=True)
    o = jnp.dot(p.astype(jnp.bfloat16), keys, preferred_element_type=jnp.float32)
    return o / total


def attend_kernel(dims, group, q_ref, kv_ref, out_ref, buf, *sems):
    net = Net(dims)
    greet(net, (net.at(x=net.ox),))
    gather_kv(net, kv_ref, buf, *sems)
    heads, rows, pair = q_ref.shape
    total = buf.shape[0] * buf.shape[1] * buf.shape[2]
    block = 128 if rows % 128 == 0 else rows
    low = lax.broadcasted_iota(jnp.int32, (block, pair), 1) < pair // 2

    def step(j, carry):
        g = j // (group // 2)
        keys = buf[:, :, :, pl.ds(pl.multiple_of(g * pair, pair), pair)].reshape(total, pair)
        for i in range(rows // block):
            at = pl.ds(i * block, block)
            a = softmax_rows(q_ref[2 * j, at, :], keys, pair // 2)
            b = softmax_rows(q_ref[2 * j + 1, at, :], keys, pair // 2)
            out_ref[at, pl.ds(pl.multiple_of(j * pair, pair), pair)] = jnp.where(
                low, pltpu.roll(a, pair // 2, 1), b
            ).astype(out_ref.dtype)
        return carry

    lax.fori_loop(0, heads // 2, step, 0)


def vmem():
    return pl.BlockSpec(memory_space=pltpu.VMEM)


def fast(dims, tokens, q_weight, k_weight, v_weight, out_weight, q_gain, k_gain):
    zs, xs, ys = dims
    rows_in = tokens[0]
    tok_count, depth = rows_in.shape
    head_width = q_gain.shape[0]
    q_heads = out_weight.shape[0] // head_width
    kv_width = k_weight.shape[1]
    group = q_heads // (kv_width // head_width)
    offset = lax.axis_index("sp") * tok_count
    width = 4 * head_width
    cos, sin = tables(tok_count, head_width, offset, width)
    own = jnp.concatenate([k_weight, v_weight, q_weight], axis=1)
    pair = 2 * head_width
    dma = pltpu.SemaphoreType.DMA
    n = 1 + 2 * (zs - 1)
    out_full = lax.all_gather(out_weight, ("sp", "dp"), axis=1, tiled=True)
    q, kv = pl.pallas_call(
        functools.partial(project_kernel, dims, head_width ** (-0.5), head_width),
        out_shape=(
            jax.ShapeDtypeStruct((q_heads, tok_count, pair), jnp.bfloat16),
            jax.ShapeDtypeStruct((tok_count, 2 * kv_width), jnp.bfloat16),
        ),
        in_specs=[vmem()] * 6,
        out_specs=(vmem(), vmem()),
        scratch_shapes=[
            pltpu.VMEM((zs, xs, ys, CORES) + own.shape, jnp.bfloat16),
            dma,
            dma((n,)), dma((n,)), dma((n,)), dma((n,)), dma((n,)), dma((n,)),
            dma((2, n)), dma((2, n)), dma((5, n)), dma((5, n)),
        ],
        compiler_params=pltpu.CompilerParams(
            collective_id=0, has_side_effects=True, vmem_limit_bytes=VMEM_BYTES
        ),
        cost_estimate=pl.CostEstimate(
            flops=60_000_000_000, bytes_accessed=10_000_000, transcendentals=0
        ),
    )(
        rows_in, own, cos, sin,
        jnp.tile(q_gain, width // head_width)[None], jnp.tile(k_gain, width // head_width)[None],
    )
    attended = pl.pallas_call(
        functools.partial(attend_kernel, dims, group),
        out_shape=jax.ShapeDtypeStruct((tok_count, q_heads * head_width), jnp.bfloat16),
        in_specs=[vmem()] * 2,
        out_specs=vmem(),
        scratch_shapes=[
            pltpu.VMEM((zs, xs) + kv.shape, jnp.bfloat16),
            dma,
            dma((n,)), dma((n,)), dma((n,)), dma((n,)),
        ],
        compiler_params=pltpu.CompilerParams(
            collective_id=1, has_side_effects=True, vmem_limit_bytes=VMEM_BYTES
        ),
        cost_estimate=pl.CostEstimate(
            flops=60_000_000_000, bytes_accessed=10_000_000, transcendentals=20_000_000
        ),
    )(q, kv)
    result = jnp.dot(attended, out_full, preferred_element_type=jnp.float32)
    return result.astype(jnp.bfloat16)[None]


def normalize(tensor, gain_vec):
    mean_sq = jnp.mean(tensor * tensor, axis=-1, keepdims=True)
    return tensor * lax.rsqrt(mean_sq + epsilon) * gain_vec


def rotate(tensor, offset):
    row_count = tensor.shape[0]
    head_width = tensor.shape[2]
    quarter = head_width // 4
    half_width = head_width // 2
    positions = jnp.arange(row_count, dtype=jnp.int32) + offset
    frequency = rope_base ** (-jnp.arange(quarter, dtype=jnp.float32) / quarter)

    def rotate_pair(segment, coords):
        angles = coords.astype(jnp.float32)[:, None] * frequency[None, :]
        cosine = jnp.cos(angles)[:, None, :]
        sine_val = jnp.sin(angles)[:, None, :]
        low_half = segment[..., :quarter]
        high_half = segment[..., quarter:]
        return jnp.concatenate(
            [low_half * cosine - high_half * sine_val, high_half * cosine + low_half * sine_val],
            axis=-1,
        )

    return jnp.concatenate(
        [
            rotate_pair(tensor[..., :half_width], positions // GRID_W),
            rotate_pair(tensor[..., half_width:], positions % GRID_W),
        ],
        axis=-1,
    )


def attend(query_rows, key_rows, value_rows):
    row_count, head_width = query_rows.shape
    block_rows = math.gcd(row_count, 512)
    score_scale = head_width ** (-0.5)

    def attend_block(segment):
        scores = (
            lax.dot_general(
                segment, key_rows, (((1,), (1,)), ((), ())), preferred_element_type=jnp.float32
            )
            * score_scale
        )
        row_max = jnp.max(scores, axis=-1, keepdims=True)
        weights = jnp.exp(scores - row_max)
        shares = (weights / jnp.sum(weights, axis=-1, keepdims=True)).astype(jnp.bfloat16)
        return jnp.dot(shares, value_rows, preferred_element_type=jnp.float32).astype(jnp.bfloat16)

    blocks = query_rows.reshape(row_count // block_rows, block_rows, head_width)
    return lax.map(attend_block, blocks).reshape(row_count, head_width)


def plain(tokens, q_weight, k_weight, v_weight, out_weight, q_gain, k_gain):
    rows_in = tokens[0]
    tok_count = rows_in.shape[0]
    head_width = q_gain.shape[0]
    q_width = out_weight.shape[0]
    kv_width = k_weight.shape[1]
    q_heads = q_width // head_width
    kv_heads = kv_width // head_width
    group_size = q_heads // kv_heads
    sp_count = lax.axis_size("sp")
    offset = lax.axis_index("sp") * tok_count
    weight_rows = (
        lax.all_gather(q_weight, ("sp", "dp"), axis=0, tiled=True),
        lax.all_gather(k_weight, ("sp", "dp"), axis=0, tiled=True),
        lax.all_gather(v_weight, ("sp", "dp"), axis=0, tiled=True),
    )
    query_raw, key_raw, value_raw = tuple(
        (
            jnp.dot(rows_in, rows_part, preferred_element_type=jnp.float32)
            for rows_part in weight_rows
        )
    )
    queries = rotate(
        normalize(query_raw.reshape(tok_count, q_heads, head_width), q_gain), offset
    ).astype(jnp.bfloat16)
    keys_rot = rotate(
        normalize(key_raw.reshape(tok_count, kv_heads, head_width), k_gain), offset
    ).astype(jnp.bfloat16)
    values_dev = value_raw.astype(jnp.bfloat16)
    keys_wide = jnp.broadcast_to(
        keys_rot[:, :, None, :], (tok_count, kv_heads, group_size, head_width)
    ).reshape(tok_count, q_width)
    values_wide = jnp.broadcast_to(
        values_dev.reshape(tok_count, kv_heads, 1, head_width),
        (tok_count, kv_heads, group_size, head_width),
    ).reshape(tok_count, q_width)
    q_local, k_local, v_local = (
        lax.all_to_all(
            queries.reshape(tok_count, q_width), "sp", split_axis=1, concat_axis=0, tiled=True
        ),
        lax.all_to_all(keys_wide, "sp", split_axis=1, concat_axis=0, tiled=True),
        lax.all_to_all(values_wide, "sp", split_axis=1, concat_axis=0, tiled=True),
    )
    local_heads = q_width // sp_count // head_width
    outputs = []
    for head_index in range(local_heads):
        low_col = head_index * head_width
        outputs.append(
            attend(
                q_local[:, low_col : low_col + head_width],
                k_local[:, low_col : low_col + head_width],
                v_local[:, low_col : low_col + head_width],
            )
        )
    head_results = jnp.concatenate(outputs, axis=1)
    attended = lax.all_to_all(head_results, "sp", split_axis=0, concat_axis=1, tiled=True)
    result = jnp.dot(
        attended,
        lax.all_gather(out_weight, ("sp", "dp"), axis=1, tiled=True),
        preferred_element_type=jnp.float32,
    ).astype(jnp.bfloat16)
    return result[None]


def solution(mesh):
    sp, dp = mesh.shape["sp"], mesh.shape["dp"]
    across = dp // CORES
    exchange = dp == 2 * CORES and sp % across == 0 and sp // across > 1
    body = functools.partial(fast, (sp // across, across, across)) if exchange else plain
    return jax.shard_map(
        body,
        mesh=mesh,
        in_specs=(
            P("dp", "sp", None),
            P(("sp", "dp"), None),
            P(("sp", "dp"), None),
            P(("sp", "dp"), None),
            P(None, ("sp", "dp")),
            P(),
            P(),
        ),
        out_specs=P("dp", "sp", None),
        check_vma=False,
    )
```

```python
import functools
import math

import jax
import jax.numpy as jnp
from jax import lax
from jax.experimental import pallas as pl
from jax.experimental.pallas import tpu as pltpu
from jax.sharding import PartitionSpec as P

GRID_W = 64
CORES = 2
epsilon = 1e-06
rope_base = 10000.0
VMEM_BYTES = 60 * 1024 * 1024


def tables(tok_count, head_width, offset, width):
    quarter = head_width // 4
    positions = jnp.arange(tok_count, dtype=jnp.int32) + offset
    frequency = rope_base ** (-jnp.arange(quarter, dtype=jnp.float32) / quarter)
    row_angle = (positions // GRID_W).astype(jnp.float32)[:, None] * frequency[None, :]
    col_angle = (positions % GRID_W).astype(jnp.float32)[:, None] * frequency[None, :]
    cos = jnp.concatenate([jnp.cos(row_angle)] * 2 + [jnp.cos(col_angle)] * 2, axis=1)
    sin_r, sin_c = jnp.sin(row_angle), jnp.sin(col_angle)
    sin = jnp.concatenate([-sin_r, sin_r, -sin_c, sin_c], axis=1)
    return jnp.tile(cos, (1, width // head_width)), jnp.tile(sin, (1, width // head_width))


class Net:
    def __init__(self, dims):
        self.zs, self.xs, self.ys = dims
        sp, dp = lax.axis_index("sp"), lax.axis_index("dp")
        self.z, self.x = sp // self.xs, sp % self.xs
        self.y, self.c = dp // CORES, dp % CORES
        self.ox, self.oy, self.oc = 1 - self.x, 1 - self.y, 1 - self.c

    def at(self, z=None, x=None, y=None, c=None):
        z = self.z if z is None else z
        x = self.x if x is None else x
        y = self.y if y is None else y
        c = self.c if c is None else c
        return {"sp": z * self.xs + x, "dp": y * CORES + c}

    def sides(self):
        return ((-1, 1), (1, -1))

    def inside(self, z):
        return jnp.logical_and(z >= 0, z < self.zs)


def greet(net, fixed):
    barrier = pltpu.get_barrier_semaphore()
    for where in fixed:
        pl.semaphore_signal(barrier, inc=1, device_id=where, device_id_type=pl.DeviceIdType.MESH)
    for step in (-1, 1):

        @pl.when(net.inside(net.z + step))
        def _():
            pl.semaphore_signal(
                barrier,
                inc=1,
                device_id=net.at(z=net.z + step),
                device_id_type=pl.DeviceIdType.MESH,
            )

    along = jnp.minimum(net.z, 1) + jnp.minimum(net.zs - 1 - net.z, 1)
    pl.semaphore_wait(barrier, len(fixed) + along)


def remote(src, dst, send, recv, where):
    return pltpu.make_async_remote_copy(
        src_ref=src,
        dst_ref=dst,
        send_sem=send,
        recv_sem=recv,
        device_id=where,
        device_id_type=pl.DeviceIdType.MESH,
    )


def gather_weights(net, w_own, wbuf, own_sem, zs_sem, zr_sem, xs, xr, ys, yr, ds, dr, cs, cr):
    half = wbuf.shape[-1] // 2
    halves = (pl.ds(0, half), pl.ds(half, half))

    def block(z, x, y, c):
        return wbuf.at[z, x, y, c]

    def part(z, x, y, c, h):
        return wbuf.at[z, x, y, c, :, halves[h]]

    def to_x(k, z, src=None):
        dst = block(z, net.x, net.y, net.c)
        return remote(dst if src is None else src, dst, xs.at[k], xr.at[k], net.at(x=net.ox))

    def from_x(k, z):
        b = block(z, net.ox, net.y, net.c)
        return remote(b, b, xs.at[k], xr.at[k], net.at(x=net.ox))

    def to_y(k, z, src=None):
        dst = block(z, net.x, net.y, net.c)
        return remote(dst if src is None else src, dst, ys.at[k], yr.at[k], net.at(y=net.oy))

    def from_y(k, z):
        b = block(z, net.x, net.oy, net.c)
        return remote(b, b, ys.at[k], yr.at[k], net.at(y=net.oy))

    def diag_to(k, z, h):
        if h == 0:
            b = part(z, net.ox, net.y, net.c, 0)
            return remote(b, b, ds.at[0, k], dr.at[0, k], net.at(y=net.oy))
        b = part(z, net.x, net.oy, net.c, 1)
        return remote(b, b, ds.at[1, k], dr.at[1, k], net.at(x=net.ox))

    def diag_from(k, z, h):
        b = part(z, net.ox, net.oy, net.c, h)
        where = net.at(y=net.oy) if h == 0 else net.at(x=net.ox)
        return remote(b, b, ds.at[h, k], dr.at[h, k], where)

    def core(kind, k, z, c, src=None):
        x = net.ox if kind in (1, 3, 4) else net.x
        y = net.oy if kind in (2, 3, 4) else net.y
        b = part(z, x, y, c, kind - 3) if kind >= 3 else block(z, x, y, c)
        return remote(
            b if src is None else src, b, cs.at[kind, k], cr.at[kind, k], net.at(c=net.oc)
        )

    def to_z(k, z, step, src=None):
        dst = block(z, net.x, net.y, net.c)
        return remote(
            dst if src is None else src, dst, zs_sem.at[k], zr_sem.at[k], net.at(z=net.z + step)
        )

    def slots():
        for step in range(net.zs - 1):
            for side in range(2):
                sign = -1 if side == 0 else 1
                yield step, side, 1 + 2 * step + side, net.z + sign * (step + 1), -sign

    def spread(k, z, src=None):
        to_x(k, z, src).start()
        to_y(k, z, src).start()
        core(0, k, z, net.c, src).start()

    def second(k, z):
        from_x(k, z).wait_recv()
        diag_to(k, z, 0).start()
        core(1, k, z, net.c).start()
        from_y(k, z).wait_recv()
        diag_to(k, z, 1).start()
        core(2, k, z, net.c).start()

    def third(k, z):
        diag_from(k, z, 0).wait_recv()
        core(3, k, z, net.c).start()
        diag_from(k, z, 1).wait_recv()
        core(4, k, z, net.c).start()

    mine = pltpu.make_async_copy(w_own, block(net.z, net.x, net.y, net.c), own_sem)
    mine.start()
    for side, step in ((0, 1), (1, -1)):

        @pl.when(net.inside(net.z + step))
        def _():
            to_z(1 + side, net.z, step, w_own).start()

    spread(0, net.z, w_own)
    stages = [[(0, net.z)]]
    for s in range(net.zs - 1):
        here = []
        for step, side, k, z, onward in slots():
            if step != s:
                continue

            @pl.when(net.inside(z))
            def _():
                to_z(k, z, 0).wait_recv()
                if s < net.zs - 2:

                    @pl.when(net.inside(net.z + onward))
                    def _():
                        to_z(k + 2, z, onward).start()

                spread(k, z)

            here.append((k, z))
        for k, z in stages[-1]:

            @pl.when(net.inside(z))
            def _():
                second(k, z)

        if len(stages) > 1:
            for k, z in stages[-2]:

                @pl.when(net.inside(z))
                def _():
                    third(k, z)

        stages.append(here)
    for k, z in stages[-1]:

        @pl.when(net.inside(z))
        def _():
            second(k, z)

    for stage in stages[-2:]:
        for k, z in stage:

            @pl.when(net.inside(z))
            def _():
                third(k, z)

    for stage in stages:
        for k, z in stage:

            @pl.when(net.inside(z))
            def _():
                for kind in range(5):
                    core(kind, k, z, net.oc).wait_recv()

    def drain():
        mine.wait()
        for side, step in ((0, 1), (1, -1)):

            @pl.when(net.inside(net.z + step))
            def _():
                to_z(1 + side, net.z, step, w_own).wait_send()

        for step, side, k, z, onward in slots():
            if step < net.zs - 2:

                @pl.when(jnp.logical_and(net.inside(z), net.inside(net.z + onward)))
                def _():
                    to_z(k + 2, z, onward).wait_send()

        for stage in stages:
            for k, z in stage:

                @pl.when(net.inside(z))
                def _():
                    to_x(k, z).wait_send()
                    to_y(k, z).wait_send()
                    diag_to(k, z, 0).wait_send()
                    diag_to(k, z, 1).wait_send()
                    for kind in range(5):
                        core(kind, k, z, net.c).wait_send()

    drain()


def exchange(net, own, buf, own_sem, zs_sem, zr_sem, xs, xr):
    last = 2 * (net.zs - 1)

    def block(z, x):
        return buf.at[z, x]

    def to_z(k, z, step, src=None):
        dst = block(z, net.x)
        return remote(
            dst if src is None else src, dst, zs_sem.at[k], zr_sem.at[k], net.at(z=net.z + step)
        )

    def to_x(k, z, src=None):
        dst = block(z, net.x)
        return remote(dst if src is None else src, dst, xs.at[k], xr.at[k], net.at(x=net.ox))

    def from_x(k, z):
        b = block(z, net.ox)
        return remote(b, b, xs.at[k], xr.at[k], net.at(x=net.ox))

    def owner(k):
        return net.z + jnp.where(k % 2 == 1, -1, 1) * ((k + 1) // 2)

    def goes_on(k):
        return jnp.logical_and(k + 2 <= last, net.inside(net.z + jnp.where(k % 2 == 1, 1, -1)))

    mine = pltpu.make_async_copy(own, block(net.z, net.x), own_sem)

    def start():
        mine.start()
        for side, step in ((0, 1), (1, -1)):

            @pl.when(net.inside(net.z + step))
            def _():
                to_z(1 + side, net.z, step, own).start()

        to_x(0, net.z, own).start()

    def pass_on(k):
        z = owner(k)

        @pl.when(jnp.logical_and(k <= last, net.inside(z)))
        def _():
            to_z(k, z, 0).wait_recv()

            @pl.when(goes_on(k))
            def _():
                to_z(k + 2, z, jnp.where(k % 2 == 1, 1, -1)).start()

            to_x(k, z).start()

    def drain():
        for side, step in ((0, 1), (1, -1)):

            @pl.when(net.inside(net.z + step))
            def _():
                to_z(1 + side, net.z, step, own).wait_send()

        to_x(0, net.z, own).wait_send()

        def one(k, carry):
            z = owner(k)

            @pl.when(net.inside(z))
            def _():
                to_x(k, z).wait_send()

                @pl.when(goes_on(k))
                def _():
                    to_z(k + 2, z, jnp.where(k % 2 == 1, 1, -1)).wait_send()

            return carry

        lax.fori_loop(1, last + 1, one, 0)

    return mine, owner, from_x, start, pass_on, drain


def layer_kernel(
    dims, group, scale, head_width, tok_ref, w_own, cos_ref, sin_ref, qg_ref, kg_ref, out_ref,
    wbuf, q_ref, kv_ref, buf, acc_ref, max_ref, sum_ref, *sems
):
    net = Net(dims)
    greet(net, (net.at(x=net.ox), net.at(y=net.oy), net.at(c=net.oc)))
    gather_weights(net, w_own, wbuf, *sems[:11])
    mine, owner, from_x, start, pass_on, drain = exchange(net, kv_ref, buf, *sems[11:])
    rows, width = cos_ref.shape
    depth = tok_ref.shape[1]
    kv_width = kv_ref.shape[1] // 2
    pair = 2 * head_width
    r = lax.broadcasted_iota(jnp.int32, (width, width), 0) // head_width
    c = lax.broadcasted_iota(jnp.int32, (width, width), 1) // head_width
    averager = jnp.where(r == c, 1.0 / head_width, 0.0).astype(jnp.float32)
    lane = lax.broadcasted_iota(jnp.int32, (rows, width), 1)
    first = lane % (head_width // 2) < head_width // 4
    low = lax.broadcasted_iota(jnp.int32, (rows, pair), 1) < head_width

    def product(at):
        w = wbuf[:, :, :, :, :, at : at + width].reshape(depth, width)
        return jnp.dot(tok_ref[...], w, preferred_element_type=jnp.float32)

    def turned(t, gain):
        mean_sq = jnp.dot(
            t * t, averager, precision=lax.Precision.HIGHEST, preferred_element_type=jnp.float32
        )
        t = t * lax.rsqrt(mean_sq + epsilon) * gain
        quarter = head_width // 4
        other = jnp.where(first, pltpu.roll(t, width - quarter, 1), pltpu.roll(t, quarter, 1))
        return t * cos_ref[...] + other * sin_ref[...]

    per = width // head_width
    for j in range(kv_width // width):
        k = turned(product(j * width), kg_ref[...])
        v = product(kv_width + j * width)
        for i in range(0, per, 2):
            kp = k[:, i * head_width : i * head_width + pair]
            vp = v[:, i * head_width : i * head_width + pair]
            at = (j * per + i) * pair
            kv_ref[:, at : at + pair] = jnp.where(low, kp, pltpu.roll(vp, head_width, 1)).astype(
                kv_ref.dtype
            )
            kv_ref[:, at + pair : at + 2 * pair] = jnp.where(
                low, pltpu.roll(kp, head_width, 1), vp
            ).astype(kv_ref.dtype)
    max_ref[...] = jnp.full_like(max_ref, -jnp.inf)
    sum_ref[...] = jnp.zeros_like(sum_ref)
    acc_ref[...] = jnp.zeros_like(acc_ref)
    for j in range(q_ref.shape[0] // per):
        if j == 1:
            start()
        q = turned(product(2 * kv_width + j * width), qg_ref[...])
        q = q.astype(q_ref.dtype).astype(jnp.float32) * scale
        for i in range(0, per, 2):
            qp = q[:, i * head_width : i * head_width + pair]
            q_ref[j * per + i] = jnp.where(low, qp, 0.0).astype(q_ref.dtype)
            q_ref[j * per + i + 1] = jnp.where(low, pltpu.roll(qp, head_width, 1), 0.0).astype(
                q_ref.dtype
            )

    block = 128 if rows % 128 == 0 else rows
    blocks = [pl.ds(i * block, block) for i in range(rows // block)]
    keys_now = buf.shape[1] * rows
    pairs = q_ref.shape[0] // 2

    def update(h, at, keys):
        s = lax.dot_general(
            q_ref[h, at, :], keys, (((1,), (1,)), ((), ())), preferred_element_type=jnp.float32
        )
        old = max_ref[h, at, :]
        top = jnp.maximum(old, jnp.max(s, axis=-1, keepdims=True))
        p = jnp.exp(s - jnp.concatenate([top] * (keys_now // pair), axis=1))
        fade = jnp.exp(old - top)
        max_ref[h, at, :] = top
        sum_ref[h, at, :] = sum_ref[h, at, :] * fade + jnp.sum(p, axis=-1, keepdims=True)
        acc_ref[h, at, :] = acc_ref[h, at, :] * fade + jnp.dot(
            p.astype(keys.dtype), keys, preferred_element_type=jnp.float32
        )

    def attend(z):
        def step(j, carry):
            g = j // (group // 2)
            keys = buf[z, :, :, pl.ds(pl.multiple_of(g * pair, pair), pair)]
            keys = keys.reshape(keys_now, pair)
            for at in blocks:
                update(2 * j, at, keys)
                update(2 * j + 1, at, keys)
            return carry

        lax.fori_loop(0, pairs, step, 0)

    pass_on(1)
    pass_on(2)
    mine.wait()

    def arrival(k, carry):
        @pl.when(k % 2 == 1)
        def _():
            pass_on(k + 2)
            pass_on(k + 3)

        z = owner(k)

        @pl.when(net.inside(z))
        def _():
            from_x(k, z).wait_recv()
            attend(z)

        return carry

    lax.fori_loop(0, 2 * (net.zs - 1) + 1, arrival, 0)
    low_block = lax.broadcasted_iota(jnp.int32, (block, pair), 1) < head_width

    def finish(j, carry):
        for at in blocks:
            a = acc_ref[2 * j, at, :] / sum_ref[2 * j, at, :]
            b = acc_ref[2 * j + 1, at, :] / sum_ref[2 * j + 1, at, :]
            out_ref[at, pl.ds(pl.multiple_of(j * pair, pair), pair)] = jnp.where(
                low_block, pltpu.roll(a, head_width, 1), b
            ).astype(out_ref.dtype)
        return carry

    lax.fori_loop(0, pairs, finish, 0)
    drain()


def vmem():
    return pl.BlockSpec(memory_space=pltpu.VMEM)


def fast(dims, tokens, q_weight, k_weight, v_weight, out_weight, q_gain, k_gain):
    zs, xs, ys = dims
    rows_in = tokens[0]
    tok_count, depth = rows_in.shape
    head_width = q_gain.shape[0]
    q_heads = out_weight.shape[0] // head_width
    kv_width = k_weight.shape[1]
    group = q_heads // (kv_width // head_width)
    offset = lax.axis_index("sp") * tok_count
    width = 4 * head_width
    cos, sin = tables(tok_count, head_width, offset, width)
    own = jnp.concatenate([k_weight, v_weight, q_weight], axis=1)
    pair = 2 * head_width
    dma = pltpu.SemaphoreType.DMA
    n = 1 + 2 * (zs - 1)
    out_full = lax.all_gather(out_weight, ("sp", "dp"), axis=1, tiled=True)
    attended = pl.pallas_call(
        functools.partial(layer_kernel, dims, group, head_width ** (-0.5), head_width),
        out_shape=jax.ShapeDtypeStruct((tok_count, q_heads * head_width), jnp.bfloat16),
        in_specs=[vmem()] * 6,
        out_specs=vmem(),
        scratch_shapes=[
            pltpu.VMEM((zs, xs, ys, CORES) + own.shape, jnp.bfloat16),
            pltpu.VMEM((q_heads, tok_count, pair), jnp.bfloat16),
            pltpu.VMEM((tok_count, 2 * kv_width), jnp.bfloat16),
            pltpu.VMEM((zs, xs, tok_count, 2 * kv_width), jnp.bfloat16),
            pltpu.VMEM((q_heads, tok_count, pair), jnp.float32),
            pltpu.VMEM((q_heads, tok_count, pair), jnp.float32),
            pltpu.VMEM((q_heads, tok_count, pair), jnp.float32),
            dma,
            dma((n,)), dma((n,)), dma((n,)), dma((n,)), dma((n,)), dma((n,)),
            dma((2, n)), dma((2, n)), dma((5, n)), dma((5, n)),
            dma,
            dma((n,)), dma((n,)), dma((n,)), dma((n,)),
        ],
        compiler_params=pltpu.CompilerParams(
            collective_id=0, has_side_effects=True, vmem_limit_bytes=VMEM_BYTES
        ),
        cost_estimate=pl.CostEstimate(
            flops=100_000_000_000, bytes_accessed=10_000_000, transcendentals=20_000_000
        ),
    )(
        rows_in, own, cos, sin,
        jnp.tile(q_gain, width // head_width)[None], jnp.tile(k_gain, width // head_width)[None],
    )
    result = jnp.dot(attended, out_full, preferred_element_type=jnp.float32)
    return result.astype(jnp.bfloat16)[None]


def normalize(tensor, gain_vec):
    mean_sq = jnp.mean(tensor * tensor, axis=-1, keepdims=True)
    return tensor * lax.rsqrt(mean_sq + epsilon) * gain_vec


def rotate(tensor, offset):
    row_count = tensor.shape[0]
    head_width = tensor.shape[2]
    quarter = head_width // 4
    half_width = head_width // 2
    positions = jnp.arange(row_count, dtype=jnp.int32) + offset
    frequency = rope_base ** (-jnp.arange(quarter, dtype=jnp.float32) / quarter)

    def rotate_pair(segment, coords):
        angles = coords.astype(jnp.float32)[:, None] * frequency[None, :]
        cosine = jnp.cos(angles)[:, None, :]
        sine_val = jnp.sin(angles)[:, None, :]
        low_half = segment[..., :quarter]
        high_half = segment[..., quarter:]
        return jnp.concatenate(
            [low_half * cosine - high_half * sine_val, high_half * cosine + low_half * sine_val],
            axis=-1,
        )

    return jnp.concatenate(
        [
            rotate_pair(tensor[..., :half_width], positions // GRID_W),
            rotate_pair(tensor[..., half_width:], positions % GRID_W),
        ],
        axis=-1,
    )


def attend(query_rows, key_rows, value_rows):
    row_count, head_width = query_rows.shape
    block_rows = math.gcd(row_count, 512)
    score_scale = head_width ** (-0.5)

    def attend_block(segment):
        scores = (
            lax.dot_general(
                segment, key_rows, (((1,), (1,)), ((), ())), preferred_element_type=jnp.float32
            )
            * score_scale
        )
        row_max = jnp.max(scores, axis=-1, keepdims=True)
        weights = jnp.exp(scores - row_max)
        shares = (weights / jnp.sum(weights, axis=-1, keepdims=True)).astype(jnp.bfloat16)
        return jnp.dot(shares, value_rows, preferred_element_type=jnp.float32).astype(jnp.bfloat16)

    blocks = query_rows.reshape(row_count // block_rows, block_rows, head_width)
    return lax.map(attend_block, blocks).reshape(row_count, head_width)


def plain(tokens, q_weight, k_weight, v_weight, out_weight, q_gain, k_gain):
    rows_in = tokens[0]
    tok_count = rows_in.shape[0]
    head_width = q_gain.shape[0]
    q_width = out_weight.shape[0]
    kv_width = k_weight.shape[1]
    q_heads = q_width // head_width
    kv_heads = kv_width // head_width
    group_size = q_heads // kv_heads
    sp_count = lax.axis_size("sp")
    offset = lax.axis_index("sp") * tok_count
    weight_rows = (
        lax.all_gather(q_weight, ("sp", "dp"), axis=0, tiled=True),
        lax.all_gather(k_weight, ("sp", "dp"), axis=0, tiled=True),
        lax.all_gather(v_weight, ("sp", "dp"), axis=0, tiled=True),
    )
    query_raw, key_raw, value_raw = tuple(
        (
            jnp.dot(rows_in, rows_part, preferred_element_type=jnp.float32)
            for rows_part in weight_rows
        )
    )
    queries = rotate(
        normalize(query_raw.reshape(tok_count, q_heads, head_width), q_gain), offset
    ).astype(jnp.bfloat16)
    keys_rot = rotate(
        normalize(key_raw.reshape(tok_count, kv_heads, head_width), k_gain), offset
    ).astype(jnp.bfloat16)
    values_dev = value_raw.astype(jnp.bfloat16)
    keys_wide = jnp.broadcast_to(
        keys_rot[:, :, None, :], (tok_count, kv_heads, group_size, head_width)
    ).reshape(tok_count, q_width)
    values_wide = jnp.broadcast_to(
        values_dev.reshape(tok_count, kv_heads, 1, head_width),
        (tok_count, kv_heads, group_size, head_width),
    ).reshape(tok_count, q_width)
    q_local, k_local, v_local = (
        lax.all_to_all(
            queries.reshape(tok_count, q_width), "sp", split_axis=1, concat_axis=0, tiled=True
        ),
        lax.all_to_all(keys_wide, "sp", split_axis=1, concat_axis=0, tiled=True),
        lax.all_to_all(values_wide, "sp", split_axis=1, concat_axis=0, tiled=True),
    )
    local_heads = q_width // sp_count // head_width
    outputs = []
    for head_index in range(local_heads):
        low_col = head_index * head_width
        outputs.append(
            attend(
                q_local[:, low_col : low_col + head_width],
                k_local[:, low_col : low_col + head_width],
                v_local[:, low_col : low_col + head_width],
            )
        )
    head_results = jnp.concatenate(outputs, axis=1)
    attended = lax.all_to_all(head_results, "sp", split_axis=0, concat_axis=1, tiled=True)
    result = jnp.dot(
        attended,
        lax.all_gather(out_weight, ("sp", "dp"), axis=1, tiled=True),
        preferred_element_type=jnp.float32,
    ).astype(jnp.bfloat16)
    return result[None]


def solution(mesh):
    sp, dp = mesh.shape["sp"], mesh.shape["dp"]
    across = dp // CORES
    exchange = dp == 2 * CORES and sp % across == 0 and sp // across > 1
    body = functools.partial(fast, (sp // across, across, across)) if exchange else plain
    return jax.shard_map(
        body,
        mesh=mesh,
        in_specs=(
            P("dp", "sp", None),
            P(("sp", "dp"), None),
            P(("sp", "dp"), None),
            P(("sp", "dp"), None),
            P(None, ("sp", "dp")),
            P(),
            P(),
        ),
        out_specs=P("dp", "sp", None),
        check_vma=False,
    )
```

```python
import functools
import math

import jax
import jax.numpy as jnp
from jax import lax
from jax.experimental import pallas as pl
from jax.experimental.pallas import tpu as pltpu
from jax.sharding import PartitionSpec as P

GRID_W = 64
CORES = 2
epsilon = 1e-06
rope_base = 10000.0
VMEM_BYTES = 60 * 1024 * 1024


def tables(tok_count, head_width, offset, width):
    quarter = head_width // 4
    positions = jnp.arange(tok_count, dtype=jnp.int32) + offset
    frequency = rope_base ** (-jnp.arange(quarter, dtype=jnp.float32) / quarter)
    row_angle = (positions // GRID_W).astype(jnp.float32)[:, None] * frequency[None, :]
    col_angle = (positions % GRID_W).astype(jnp.float32)[:, None] * frequency[None, :]
    cos = jnp.concatenate([jnp.cos(row_angle)] * 2 + [jnp.cos(col_angle)] * 2, axis=1)
    sin_r, sin_c = jnp.sin(row_angle), jnp.sin(col_angle)
    sin = jnp.concatenate([-sin_r, sin_r, -sin_c, sin_c], axis=1)
    return jnp.tile(cos, (1, width // head_width)), jnp.tile(sin, (1, width // head_width))


class Net:
    def __init__(self, dims):
        self.zs, self.xs, self.ys = dims
        sp, dp = lax.axis_index("sp"), lax.axis_index("dp")
        self.z, self.x = sp // self.xs, sp % self.xs
        self.y, self.c = dp // CORES, dp % CORES
        self.ox, self.oy, self.oc = 1 - self.x, 1 - self.y, 1 - self.c

    def at(self, z=None, x=None, y=None, c=None):
        z = self.z if z is None else z
        x = self.x if x is None else x
        y = self.y if y is None else y
        c = self.c if c is None else c
        return {"sp": z * self.xs + x, "dp": y * CORES + c}

    def sides(self):
        return ((-1, 1), (1, -1))

    def inside(self, z):
        return jnp.logical_and(z >= 0, z < self.zs)


def greet(net, fixed):
    barrier = pltpu.get_barrier_semaphore()
    for where in fixed:
        pl.semaphore_signal(barrier, inc=1, device_id=where, device_id_type=pl.DeviceIdType.MESH)
    for step in (-1, 1):

        @pl.when(net.inside(net.z + step))
        def _():
            pl.semaphore_signal(
                barrier,
                inc=1,
                device_id=net.at(z=net.z + step),
                device_id_type=pl.DeviceIdType.MESH,
            )

    along = jnp.minimum(net.z, 1) + jnp.minimum(net.zs - 1 - net.z, 1)
    pl.semaphore_wait(barrier, len(fixed) + along)


def remote(src, dst, send, recv, where):
    return pltpu.make_async_remote_copy(
        src_ref=src,
        dst_ref=dst,
        send_sem=send,
        recv_sem=recv,
        device_id=where,
        device_id_type=pl.DeviceIdType.MESH,
    )


def gather_weights(net, w_own, wbuf, own_sem, zs_sem, zr_sem, xs, xr, ys, yr, ds, dr, cs, cr):
    half = wbuf.shape[-1] // 2
    halves = (pl.ds(0, half), pl.ds(half, half))

    def block(z, x, y, c):
        return wbuf.at[z, x, y, c]

    def part(z, x, y, c, h):
        return wbuf.at[z, x, y, c, :, halves[h]]

    def to_x(k, z, src=None):
        dst = block(z, net.x, net.y, net.c)
        return remote(dst if src is None else src, dst, xs.at[k], xr.at[k], net.at(x=net.ox))

    def from_x(k, z):
        b = block(z, net.ox, net.y, net.c)
        return remote(b, b, xs.at[k], xr.at[k], net.at(x=net.ox))

    def to_y(k, z, src=None):
        dst = block(z, net.x, net.y, net.c)
        return remote(dst if src is None else src, dst, ys.at[k], yr.at[k], net.at(y=net.oy))

    def from_y(k, z):
        b = block(z, net.x, net.oy, net.c)
        return remote(b, b, ys.at[k], yr.at[k], net.at(y=net.oy))

    def diag_to(k, z, h):
        if h == 0:
            b = part(z, net.ox, net.y, net.c, 0)
            return remote(b, b, ds.at[0, k], dr.at[0, k], net.at(y=net.oy))
        b = part(z, net.x, net.oy, net.c, 1)
        return remote(b, b, ds.at[1, k], dr.at[1, k], net.at(x=net.ox))

    def diag_from(k, z, h):
        b = part(z, net.ox, net.oy, net.c, h)
        where = net.at(y=net.oy) if h == 0 else net.at(x=net.ox)
        return remote(b, b, ds.at[h, k], dr.at[h, k], where)

    def core(kind, k, z, c, src=None):
        x = net.ox if kind in (1, 3, 4) else net.x
        y = net.oy if kind in (2, 3, 4) else net.y
        b = part(z, x, y, c, kind - 3) if kind >= 3 else block(z, x, y, c)
        return remote(
            b if src is None else src, b, cs.at[kind, k], cr.at[kind, k], net.at(c=net.oc)
        )

    def to_z(k, z, step, src=None):
        dst = block(z, net.x, net.y, net.c)
        return remote(
            dst if src is None else src, dst, zs_sem.at[k], zr_sem.at[k], net.at(z=net.z + step)
        )

    def slots():
        for step in range(net.zs - 1):
            for side in range(2):
                sign = -1 if side == 0 else 1
                yield step, side, 1 + 2 * step + side, net.z + sign * (step + 1), -sign

    def spread(k, z, src=None):
        to_x(k, z, src).start()
        to_y(k, z, src).start()
        core(0, k, z, net.c, src).start()

    def second(k, z):
        from_x(k, z).wait_recv()
        diag_to(k, z, 0).start()
        core(1, k, z, net.c).start()
        from_y(k, z).wait_recv()
        diag_to(k, z, 1).start()
        core(2, k, z, net.c).start()

    def third(k, z):
        diag_from(k, z, 0).wait_recv()
        core(3, k, z, net.c).start()
        diag_from(k, z, 1).wait_recv()
        core(4, k, z, net.c).start()

    mine = pltpu.make_async_copy(w_own, block(net.z, net.x, net.y, net.c), own_sem)
    mine.start()
    for side, step in ((0, 1), (1, -1)):

        @pl.when(net.inside(net.z + step))
        def _():
            to_z(1 + side, net.z, step, w_own).start()

    spread(0, net.z, w_own)
    stages = [[(0, net.z)]]
    for s in range(net.zs - 1):
        here = []
        for step, side, k, z, onward in slots():
            if step != s:
                continue

            @pl.when(net.inside(z))
            def _():
                to_z(k, z, 0).wait_recv()
                if s < net.zs - 2:

                    @pl.when(net.inside(net.z + onward))
                    def _():
                        to_z(k + 2, z, onward).start()

                spread(k, z)

            here.append((k, z))
        for k, z in stages[-1]:

            @pl.when(net.inside(z))
            def _():
                second(k, z)

        if len(stages) > 1:
            for k, z in stages[-2]:

                @pl.when(net.inside(z))
                def _():
                    third(k, z)

        stages.append(here)
    for k, z in stages[-1]:

        @pl.when(net.inside(z))
        def _():
            second(k, z)

    for stage in stages[-2:]:
        for k, z in stage:

            @pl.when(net.inside(z))
            def _():
                third(k, z)

    for stage in stages:
        for k, z in stage:

            @pl.when(net.inside(z))
            def _():
                for kind in range(5):
                    core(kind, k, z, net.oc).wait_recv()

    def drain():
        mine.wait()
        for side, step in ((0, 1), (1, -1)):

            @pl.when(net.inside(net.z + step))
            def _():
                to_z(1 + side, net.z, step, w_own).wait_send()

        for step, side, k, z, onward in slots():
            if step < net.zs - 2:

                @pl.when(jnp.logical_and(net.inside(z), net.inside(net.z + onward)))
                def _():
                    to_z(k + 2, z, onward).wait_send()

        for stage in stages:
            for k, z in stage:

                @pl.when(net.inside(z))
                def _():
                    to_x(k, z).wait_send()
                    to_y(k, z).wait_send()
                    diag_to(k, z, 0).wait_send()
                    diag_to(k, z, 1).wait_send()
                    for kind in range(5):
                        core(kind, k, z, net.c).wait_send()

    drain()


def exchange(net, own, buf, own_sem, zs_sem, zr_sem, xs, xr):
    last = 2 * (net.zs - 1)

    def block(z, x):
        return buf.at[z, x]

    def to_z(k, z, step, src=None):
        dst = block(z, net.x)
        return remote(
            dst if src is None else src, dst, zs_sem.at[k], zr_sem.at[k], net.at(z=net.z + step)
        )

    def to_x(k, z, src=None):
        dst = block(z, net.x)
        return remote(dst if src is None else src, dst, xs.at[k], xr.at[k], net.at(x=net.ox))

    def from_x(k, z):
        b = block(z, net.ox)
        return remote(b, b, xs.at[k], xr.at[k], net.at(x=net.ox))

    def owner(k):
        return net.z + jnp.where(k % 2 == 1, -1, 1) * ((k + 1) // 2)

    def goes_on(k):
        return jnp.logical_and(k + 2 <= last, net.inside(net.z + jnp.where(k % 2 == 1, 1, -1)))

    mine = pltpu.make_async_copy(own, block(net.z, net.x), own_sem)

    def start():
        mine.start()
        for side, step in ((0, 1), (1, -1)):

            @pl.when(net.inside(net.z + step))
            def _():
                to_z(1 + side, net.z, step, own).start()

        to_x(0, net.z, own).start()

    def pass_on(k):
        z = owner(k)

        @pl.when(jnp.logical_and(k <= last, net.inside(z)))
        def _():
            to_z(k, z, 0).wait_recv()

            @pl.when(goes_on(k))
            def _():
                to_z(k + 2, z, jnp.where(k % 2 == 1, 1, -1)).start()

            to_x(k, z).start()

    def drain():
        for side, step in ((0, 1), (1, -1)):

            @pl.when(net.inside(net.z + step))
            def _():
                to_z(1 + side, net.z, step, own).wait_send()

        to_x(0, net.z, own).wait_send()

        def one(k, carry):
            z = owner(k)

            @pl.when(net.inside(z))
            def _():
                to_x(k, z).wait_send()

                @pl.when(goes_on(k))
                def _():
                    to_z(k + 2, z, jnp.where(k % 2 == 1, 1, -1)).wait_send()

            return carry

        lax.fori_loop(1, last + 1, one, 0)

    return mine, owner, from_x, start, pass_on, drain


def layer_kernel(
    dims, group, scale, head_width, tok_ref, w_own, cos_ref, sin_ref, gain_ref, out_ref,
    wbuf, q_ref, kv_ref, buf, acc_ref, max_ref, sum_ref, *sems
):
    net = Net(dims)
    greet(net, (net.at(x=net.ox), net.at(y=net.oy), net.at(c=net.oc)))
    gather_weights(net, w_own, wbuf, *sems[:11])
    mine, owner, from_x, start, pass_on, drain = exchange(net, kv_ref, buf, *sems[11:])
    rows, width = cos_ref.shape
    depth = tok_ref.shape[1]
    kv_width = kv_ref.shape[1] // 2
    pair = 2 * head_width
    r = lax.broadcasted_iota(jnp.int32, (width, width), 0) // head_width
    c = lax.broadcasted_iota(jnp.int32, (width, width), 1) // head_width
    averager = jnp.where(r == c, 1.0 / head_width, 0.0).astype(jnp.float32)
    lane = lax.broadcasted_iota(jnp.int32, (rows, width), 1)
    first = lane % (head_width // 2) < head_width // 4
    low = lax.broadcasted_iota(jnp.int32, (rows, pair), 1) < head_width

    def product(at):
        w = wbuf[:, :, :, :, :, at : at + width].reshape(depth, width)
        return jnp.dot(tok_ref[...], w, preferred_element_type=jnp.float32)

    def turned(t, gain):
        mean_sq = jnp.dot(
            t * t, averager, precision=lax.Precision.HIGHEST, preferred_element_type=jnp.float32
        )
        t = t * lax.rsqrt(mean_sq + epsilon) * gain
        quarter = head_width // 4
        other = jnp.where(first, pltpu.roll(t, width - quarter, 1), pltpu.roll(t, quarter, 1))
        return t * cos_ref[...] + other * sin_ref[...]

    per = width // head_width
    for j in range(kv_width // width):
        k = turned(product(j * width), gain_ref[1:2, :])
        v = product(kv_width + j * width)
        for i in range(0, per, 2):
            kp = k[:, i * head_width : i * head_width + pair]
            vp = v[:, i * head_width : i * head_width + pair]
            at = (j * per + i) * pair
            kv_ref[:, at : at + pair] = jnp.where(low, kp, pltpu.roll(vp, head_width, 1)).astype(
                kv_ref.dtype
            )
            kv_ref[:, at + pair : at + 2 * pair] = jnp.where(
                low, pltpu.roll(kp, head_width, 1), vp
            ).astype(kv_ref.dtype)
    max_ref[...] = jnp.full_like(max_ref, -jnp.inf)
    sum_ref[...] = jnp.zeros_like(sum_ref)
    acc_ref[...] = jnp.zeros_like(acc_ref)
    for j in range(q_ref.shape[0] // per):
        if j == 1:
            start()
        q = turned(product(2 * kv_width + j * width), gain_ref[0:1, :])
        q = q.astype(q_ref.dtype).astype(jnp.float32) * scale
        for i in range(0, per, 2):
            qp = q[:, i * head_width : i * head_width + pair]
            q_ref[j * per + i] = jnp.where(low, qp, 0.0).astype(q_ref.dtype)
            q_ref[j * per + i + 1] = jnp.where(low, pltpu.roll(qp, head_width, 1), 0.0).astype(
                q_ref.dtype
            )

    block = 128 if rows % 128 == 0 else rows
    blocks = [pl.ds(i * block, block) for i in range(rows // block)]
    keys_now = buf.shape[1] * rows
    pairs = q_ref.shape[0] // 2

    def update(h, keys, old, total, acc):
        s = lax.dot_general(
            q_ref[h], keys, (((1,), (1,)), ((), ())), preferred_element_type=jnp.float32
        )
        top = jnp.maximum(old, jnp.max(s, axis=-1, keepdims=True))
        p = jnp.exp(s - jnp.concatenate([top] * (keys_now // pair), axis=1))
        fade = jnp.exp(old - top)
        total = total * fade + jnp.sum(p, axis=-1, keepdims=True)
        acc = acc * fade + jnp.dot(
            p.astype(keys.dtype), keys, preferred_element_type=jnp.float32
        )
        return top, total, acc

    def attend(z):
        def step(j, carry):
            g = j // (group // 2)
            keys = buf[z, :, :, pl.ds(pl.multiple_of(g * pair, pair), pair)]
            keys = keys.reshape(keys_now, pair)
            two = (2 * j, 2 * j + 1)
            state = [(max_ref[h], sum_ref[h], acc_ref[h]) for h in two]
            state = [update(h, keys, *held) for h, held in zip(two, state)]
            for h, (top, total, acc) in zip(two, state):
                max_ref[h] = top
                sum_ref[h] = total
                acc_ref[h] = acc
            return carry

        lax.fori_loop(0, pairs, step, 0)

    pass_on(1)
    pass_on(2)
    mine.wait()

    def arrival(k, carry):
        @pl.when(k % 2 == 1)
        def _():
            pass_on(k + 2)
            pass_on(k + 3)

        z = owner(k)

        @pl.when(net.inside(z))
        def _():
            from_x(k, z).wait_recv()
            attend(z)

        return carry

    lax.fori_loop(0, 2 * (net.zs - 1) + 1, arrival, 0)
    low_block = lax.broadcasted_iota(jnp.int32, (block, pair), 1) < head_width

    def finish(j, carry):
        for at in blocks:
            a = acc_ref[2 * j, at, :] / sum_ref[2 * j, at, :]
            b = acc_ref[2 * j + 1, at, :] / sum_ref[2 * j + 1, at, :]
            out_ref[at, pl.ds(pl.multiple_of(j * pair, pair), pair)] = jnp.where(
                low_block, pltpu.roll(a, head_width, 1), b
            ).astype(out_ref.dtype)
        return carry

    lax.fori_loop(0, pairs, finish, 0)
    drain()


def vmem():
    return pl.BlockSpec(memory_space=pltpu.VMEM)


def fast(dims, tokens, q_weight, k_weight, v_weight, out_weight, q_gain, k_gain):
    zs, xs, ys = dims
    rows_in = tokens[0]
    tok_count, depth = rows_in.shape
    head_width = q_gain.shape[0]
    q_heads = out_weight.shape[0] // head_width
    kv_width = k_weight.shape[1]
    group = q_heads // (kv_width // head_width)
    offset = lax.axis_index("sp") * tok_count
    width = 4 * head_width
    cos, sin = tables(tok_count, head_width, offset, width)
    own = jnp.concatenate([k_weight, v_weight, q_weight], axis=1)
    pair = 2 * head_width
    dma = pltpu.SemaphoreType.DMA
    n = 1 + 2 * (zs - 1)
    out_full = lax.all_gather(out_weight, ("sp", "dp"), axis=1, tiled=True)
    attended = pl.pallas_call(
        functools.partial(layer_kernel, dims, group, head_width ** (-0.5), head_width),
        out_shape=jax.ShapeDtypeStruct((tok_count, q_heads * head_width), jnp.bfloat16),
        in_specs=[vmem()] * 5,
        out_specs=vmem(),
        scratch_shapes=[
            pltpu.VMEM((zs, xs, ys, CORES) + own.shape, jnp.bfloat16),
            pltpu.VMEM((q_heads, tok_count, pair), jnp.bfloat16),
            pltpu.VMEM((tok_count, 2 * kv_width), jnp.bfloat16),
            pltpu.VMEM((zs, xs, tok_count, 2 * kv_width), jnp.bfloat16),
            pltpu.VMEM((q_heads, tok_count, pair), jnp.float32),
            pltpu.VMEM((q_heads, tok_count, pair), jnp.float32),
            pltpu.VMEM((q_heads, tok_count, pair), jnp.float32),
            dma,
            dma((n,)), dma((n,)), dma((n,)), dma((n,)), dma((n,)), dma((n,)),
            dma((2, n)), dma((2, n)), dma((5, n)), dma((5, n)),
            dma,
            dma((n,)), dma((n,)), dma((n,)), dma((n,)),
        ],
        compiler_params=pltpu.CompilerParams(
            collective_id=0, has_side_effects=True, vmem_limit_bytes=VMEM_BYTES
        ),
        cost_estimate=pl.CostEstimate(
            flops=100_000_000_000, bytes_accessed=10_000_000, transcendentals=20_000_000
        ),
    )(
        rows_in, own, cos, sin,
        jnp.tile(jnp.stack([q_gain, k_gain]), (1, width // head_width)),
    )
    result = jnp.dot(attended, out_full, preferred_element_type=jnp.float32)
    return result.astype(jnp.bfloat16)[None]


def normalize(tensor, gain_vec):
    mean_sq = jnp.mean(tensor * tensor, axis=-1, keepdims=True)
    return tensor * lax.rsqrt(mean_sq + epsilon) * gain_vec


def rotate(tensor, offset):
    row_count = tensor.shape[0]
    head_width = tensor.shape[2]
    quarter = head_width // 4
    half_width = head_width // 2
    positions = jnp.arange(row_count, dtype=jnp.int32) + offset
    frequency = rope_base ** (-jnp.arange(quarter, dtype=jnp.float32) / quarter)

    def rotate_pair(segment, coords):
        angles = coords.astype(jnp.float32)[:, None] * frequency[None, :]
        cosine = jnp.cos(angles)[:, None, :]
        sine_val = jnp.sin(angles)[:, None, :]
        low_half = segment[..., :quarter]
        high_half = segment[..., quarter:]
        return jnp.concatenate(
            [low_half * cosine - high_half * sine_val, high_half * cosine + low_half * sine_val],
            axis=-1,
        )

    return jnp.concatenate(
        [
            rotate_pair(tensor[..., :half_width], positions // GRID_W),
            rotate_pair(tensor[..., half_width:], positions % GRID_W),
        ],
        axis=-1,
    )


def attend(query_rows, key_rows, value_rows):
    row_count, head_width = query_rows.shape
    block_rows = math.gcd(row_count, 512)
    score_scale = head_width ** (-0.5)

    def attend_block(segment):
        scores = (
            lax.dot_general(
                segment, key_rows, (((1,), (1,)), ((), ())), preferred_element_type=jnp.float32
            )
            * score_scale
        )
        row_max = jnp.max(scores, axis=-1, keepdims=True)
        weights = jnp.exp(scores - row_max)
        shares = (weights / jnp.sum(weights, axis=-1, keepdims=True)).astype(jnp.bfloat16)
        return jnp.dot(shares, value_rows, preferred_element_type=jnp.float32).astype(jnp.bfloat16)

    blocks = query_rows.reshape(row_count // block_rows, block_rows, head_width)
    return lax.map(attend_block, blocks).reshape(row_count, head_width)


def plain(tokens, q_weight, k_weight, v_weight, out_weight, q_gain, k_gain):
    rows_in = tokens[0]
    tok_count = rows_in.shape[0]
    head_width = q_gain.shape[0]
    q_width = out_weight.shape[0]
    kv_width = k_weight.shape[1]
    q_heads = q_width // head_width
    kv_heads = kv_width // head_width
    group_size = q_heads // kv_heads
    sp_count = lax.axis_size("sp")
    offset = lax.axis_index("sp") * tok_count
    weight_rows = (
        lax.all_gather(q_weight, ("sp", "dp"), axis=0, tiled=True),
        lax.all_gather(k_weight, ("sp", "dp"), axis=0, tiled=True),
        lax.all_gather(v_weight, ("sp", "dp"), axis=0, tiled=True),
    )
    query_raw, key_raw, value_raw = tuple(
        (
            jnp.dot(rows_in, rows_part, preferred_element_type=jnp.float32)
            for rows_part in weight_rows
        )
    )
    queries = rotate(
        normalize(query_raw.reshape(tok_count, q_heads, head_width), q_gain), offset
    ).astype(jnp.bfloat16)
    keys_rot = rotate(
        normalize(key_raw.reshape(tok_count, kv_heads, head_width), k_gain), offset
    ).astype(jnp.bfloat16)
    values_dev = value_raw.astype(jnp.bfloat16)
    keys_wide = jnp.broadcast_to(
        keys_rot[:, :, None, :], (tok_count, kv_heads, group_size, head_width)
    ).reshape(tok_count, q_width)
    values_wide = jnp.broadcast_to(
        values_dev.reshape(tok_count, kv_heads, 1, head_width),
        (tok_count, kv_heads, group_size, head_width),
    ).reshape(tok_count, q_width)
    q_local, k_local, v_local = (
        lax.all_to_all(
            queries.reshape(tok_count, q_width), "sp", split_axis=1, concat_axis=0, tiled=True
        ),
        lax.all_to_all(keys_wide, "sp", split_axis=1, concat_axis=0, tiled=True),
        lax.all_to_all(values_wide, "sp", split_axis=1, concat_axis=0, tiled=True),
    )
    local_heads = q_width // sp_count // head_width
    outputs = []
    for head_index in range(local_heads):
        low_col = head_index * head_width
        outputs.append(
            attend(
                q_local[:, low_col : low_col + head_width],
                k_local[:, low_col : low_col + head_width],
                v_local[:, low_col : low_col + head_width],
            )
        )
    head_results = jnp.concatenate(outputs, axis=1)
    attended = lax.all_to_all(head_results, "sp", split_axis=0, concat_axis=1, tiled=True)
    result = jnp.dot(
        attended,
        lax.all_gather(out_weight, ("sp", "dp"), axis=1, tiled=True),
        preferred_element_type=jnp.float32,
    ).astype(jnp.bfloat16)
    return result[None]


def solution(mesh):
    sp, dp = mesh.shape["sp"], mesh.shape["dp"]
    across = dp // CORES
    exchange = dp == 2 * CORES and sp % across == 0 and sp // across > 1
    body = functools.partial(fast, (sp // across, across, across)) if exchange else plain
    return jax.shard_map(
        body,
        mesh=mesh,
        in_specs=(
            P("dp", "sp", None),
            P(("sp", "dp"), None),
            P(("sp", "dp"), None),
            P(("sp", "dp"), None),
            P(None, ("sp", "dp")),
            P(),
            P(),
        ),
        out_specs=P("dp", "sp", None),
        check_vma=False,
    )
```
